128 devices in a mesh: sp: 16 (over z, y), dp: 8 (over x, core).
Axes of the slice: x: 4, y: 4, z: 4, core: 2. Of those that a mesh axis runs over, the one named last changes fastest.
Arguments:
- tokens: bfloat16 [8, 4096, 2048], P('dp', 'sp'), may hold values from -6 to 6
- in_gain: float32 [2048], replicated, may hold values from 0.1 to 1.9
- w_query_down: bfloat16 [2048, 512], P('dp'), may hold values from -0.125 to 0.125
- w_latent_down: bfloat16 [2048, 256], P('dp'), may hold values from -0.125 to 0.125
- w_rope_key: bfloat16 [2048, 64], replicated, may hold values from -0.125 to 0.125
- query_latent_gain: float32 [512], replicated, may hold values from 0.1 to 1.9
- latent_gain: float32 [256], replicated, may hold values from 0.1 to 1.9
- w_query_up: bfloat16 [512, 3072], P('dp', 'sp'), may hold values from -0.25 to 0.25
- w_key_up: bfloat16 [256, 2048], P('dp', 'sp'), may hold values from -0.375 to 0.375
- w_value_up: bfloat16 [256, 2048], P('dp', 'sp'), may hold values from -0.375 to 0.375
- query_gain: float32 [192], replicated, may hold values from 0.5 to 14
- key_gain: float32 [192], replicated, may hold values from 0.5 to 14
- out_gain: float32 [2048], replicated, may hold values from 0.1 to 1.9
- w_out: bfloat16 [2048, 2048], P(('sp', 'dp')), may hold values from -0.125 to 0.125
Outputs:
- result: bfloat16 [8, 4096, 2048], P('dp', 'sp')
The draws below stay inside these ranges and needn't reach their ends.
All inputs are finite; a program needn't handle non-finite values.
Results may differ from the reference program's by a relative error of at most 0.034.
The reference program's roundings to bfloat16 on the way count: a program that leaves them out, or rounds other values in their place, can miss the bound.
Values may be sent and summed in bfloat16 or wider, within the bound.
No kernel may reach another device: no remote copies, remote signals or barrier semaphores. Data moves between devices by JAX's collectives and lax.ppermute only.
A program may use at most 64 MiB of HBM per device.

```python
import jax
import jax.numpy as jnp
from jax import lax

D = 2048
HEADS = 16
NOPE = 128
ROPE = 64
VD = 128
QR = 512
KR = 256
QK = 192
LEN = 4096
SEQS = 8


def gain_vector(key, member):
    spread = jnp.clip(jax.random.normal(jax.random.fold_in(key, 11 + member), (QK,), jnp.float32), -2.5, 2.5)
    return (1.0 + 0.18 * spread).astype(jnp.float32)


def draw_query_gain(key, part):
    return gain_vector(key, 0)


def draw_key_gain(key, part):
    return gain_vector(key, 1)


def block_levels(own_key, shape, split, least, largest):
    gain, own = 1.0, jax.random.fold_in(own_key, 6)
    for dim, parts in split:
        draws = jnp.exp(jax.random.uniform(jax.random.fold_in(own, dim), (parts,), jnp.float32, least / len(split), largest / len(split)))
        gain = gain * jnp.repeat(draws, shape[dim] // parts).reshape([-1 if axis == dim else 1 for axis in range(len(shape))])
    return gain


def centred(stream_key, shape, scale, limit, split=(), kind=jnp.bfloat16):
    values = jax.random.normal(stream_key, shape, jnp.float32) * scale
    if len(split) > 0:
        values = block_levels(stream_key, shape, split, -0.22, 0.18) * values
    return jnp.clip(values, min=-limit, max=limit).astype(kind)


def setup_inputs(seed: int = 0) -> dict:
    arg_keys = jax.random.split(jax.random.key(seed), 15)
    tokens = centred(arg_keys[0], (SEQS, LEN, D), 1.0, 6.0, ((0, 8), (1, 16)))
    in_gain = jnp.clip(1.0 + 0.18 * jax.random.normal(arg_keys[1], (D,), jnp.float32), 0.1, 1.9)
    w_query_down = centred(arg_keys[2], (D, QR), D ** -0.5, 0.125, ((0, 8),))
    w_latent_down = centred(arg_keys[3], (D, KR), D ** -0.5, 0.125, ((0, 8),))
    w_rope_key = centred(arg_keys[4], (D, ROPE), D ** -0.5, 0.125)
    query_latent_gain = jnp.clip(1.0 + 0.18 * jax.random.normal(arg_keys[5], (QR,), jnp.float32), 0.1, 1.9)
    latent_gain = jnp.clip(1.0 + 0.18 * jax.random.normal(arg_keys[6], (KR,), jnp.float32), 0.1, 1.9)
    w_query_up = centred(arg_keys[7], (QR, HEADS * QK), QR ** -0.5, 0.25, ((0, 8), (1, 16)))
    w_key_up = centred(arg_keys[8], (KR, HEADS * NOPE), KR ** -0.5, 0.375, ((0, 8), (1, 16)))
    w_value_up = centred(arg_keys[9], (KR, HEADS * VD), KR ** -0.5, 0.375, ((0, 8), (1, 16)))
    query_gain = draw_query_gain(jax.random.fold_in(arg_keys[14], 71), 0)
    key_gain = draw_key_gain(jax.random.fold_in(arg_keys[14], 71), 0)
    out_gain = jnp.clip(1.0 + 0.18 * jax.random.normal(arg_keys[12], (HEADS * VD,), jnp.float32), 0.1, 1.9)
    w_out = centred(arg_keys[13], (HEADS * VD, D), (HEADS * VD) ** -0.5, 0.125, ((0, 128),))
    return dict(tokens=tokens, in_gain=in_gain, w_query_down=w_query_down, w_latent_down=w_latent_down, w_rope_key=w_rope_key, query_latent_gain=query_latent_gain, latent_gain=latent_gain, w_query_up=w_query_up, w_key_up=w_key_up, w_value_up=w_value_up, query_gain=query_gain, key_gain=key_gain, out_gain=out_gain, w_out=w_out)


EPS = 1e-06
THETA = 10000.0
NEG_BIG = -1e+30

def rms_scale(values, scaling):
    return values * lax.rsqrt(lax.optimization_barrier(jnp.mean(values * values, axis=-1, keepdims=True)) + EPS) * scaling

def rotate(tail_part, positions):
    half_width = tail_part.shape[-1] // 2
    frequency = THETA ** (-jnp.arange(half_width, dtype=jnp.float32) / half_width)
    angles = positions[:, None] * frequency[None, :]
    cosine = jnp.cos(angles)[:, None, :]
    sine = jnp.sin(angles)[:, None, :]
    first_half = tail_part[..., :half_width]
    second_half = tail_part[..., half_width:]
    return jnp.concatenate([first_half * cosine - second_half * sine, second_half * cosine + first_half * sine], axis=-1)

def finish_heads(joined, positions, scaling, rope_width):
    row_count = joined.shape[0]
    normal = rms_scale(joined, scaling)
    turned = rotate(normal[..., -rope_width:], positions)
    return jnp.concatenate([normal[..., :-rope_width], turned], axis=-1).astype(jnp.bfloat16).reshape(row_count, -1)

def attend(queries, keys, values, head_count):
    length = queries.shape[0]
    block_rows = min(512, length)
    query_blocks = queries.reshape(length // block_rows, block_rows, head_count, -1)
    key_heads = keys.reshape(length, head_count, -1).astype(jnp.float32)
    value_heads = values.reshape(length, head_count, -1).astype(jnp.float32)
    score_scale = key_heads.shape[-1] ** (-0.5)
    key_pos = jnp.arange(length)

    def one_block(block_args):
        query_block, block_index = block_args
        scores = jnp.einsum('qhd,khd->hqk', query_block.astype(jnp.float32), key_heads) * score_scale
        query_pos = block_index * block_rows + jnp.arange(block_rows)
        allowed = key_pos[None, :] <= query_pos[:, None]
        scores = jnp.where(allowed[None], scores, NEG_BIG)
        weights = jax.nn.softmax(scores, axis=-1).astype(jnp.bfloat16)
        return jnp.einsum('hqk,khd->qhd', weights.astype(jnp.float32), value_heads).astype(jnp.bfloat16)
    outcome = lax.map(one_block, (query_blocks, jnp.arange(length // block_rows)))
    return outcome.reshape(length, -1)

def reference(tokens, in_gain, w_query_down, w_latent_down, w_rope_key, query_latent_gain, latent_gain, w_query_up, w_key_up, w_value_up, query_gain, key_gain, out_gain, w_out):

    def one_sequence(sequence):
        normed = rms_scale(sequence.astype(jnp.float32), in_gain).astype(jnp.bfloat16)
        latent_q = rms_scale(jnp.dot(normed, w_query_down, preferred_element_type=jnp.float32), query_latent_gain).astype(jnp.bfloat16)
        latent_kv = rms_scale(jnp.dot(normed, w_latent_down, preferred_element_type=jnp.float32), latent_gain).astype(jnp.bfloat16)
        rope_key = jnp.dot(normed, w_rope_key, preferred_element_type=jnp.float32).astype(jnp.bfloat16)
        positions = jnp.arange(LEN, dtype=jnp.float32)
        query_total = jnp.dot(latent_q, w_query_up, preferred_element_type=jnp.float32)
        queries = finish_heads(query_total.reshape(LEN, HEADS, QK), positions, query_gain, ROPE)
        key_total = jnp.dot(latent_kv, w_key_up, preferred_element_type=jnp.float32).reshape(LEN, HEADS, NOPE)
        shared = jnp.broadcast_to(rope_key.astype(jnp.float32)[:, None, :], (LEN, HEADS, ROPE))
        keys = finish_heads(jnp.concatenate([key_total, shared], axis=-1), positions, key_gain, ROPE)
        values = jnp.dot(latent_kv, w_value_up, preferred_element_type=jnp.float32).astype(jnp.bfloat16)
        attended = attend(queries, keys, values, HEADS)
        mixed = rms_scale(attended.astype(jnp.float32), out_gain).astype(jnp.bfloat16)
        return jnp.dot(mixed, w_out, preferred_element_type=jnp.float32).astype(jnp.bfloat16)
    return lax.map(one_sequence, tokens)
```

```python
import jax
import jax.numpy as jnp
from jax import lax
from jax.experimental import pallas as pl
from jax.experimental.pallas import tpu as pltpu
from jax.sharding import PartitionSpec as P


HEADS = 16
EPS = 1e-06
THETA = 10000.0
NEG_BIG = -1e30
LOG2E = 1.4426950408889634
F32 = jnp.float32
BF16 = jnp.bfloat16

RING = 4
CORES = 2
BLOCK = 256
TAIL = 64
HALF = TAIL // 2
VMEM = pltpu.VMEM
SMEM = pltpu.SMEM


def sp_pairs(dz, dy):
    return [
        (z * RING + y, (z + dz) % RING * RING + (y + dy) % RING)
        for z in range(RING)
        for y in range(RING)
    ]


def dp_pairs(dx):
    return [
        (x * CORES + c, (x + dx) % RING * CORES + c) for x in range(RING) for c in range(CORES)
    ]


def from_z(value):
    return [value] + [lax.ppermute(value, "sp", sp_pairs(k, 0)) for k in range(1, RING)]


def from_y(value):
    return [value] + [lax.ppermute(value, "sp", sp_pairs(0, k)) for k in range(1, RING)]


def from_x(value):
    return [value] + [lax.ppermute(value, "dp", dp_pairs(k)) for k in range(1, RING)]


def from_core(value):
    return lax.ppermute(
        value, "dp", [(x * CORES + c, x * CORES + 1 - c) for x in range(RING) for c in range(CORES)]
    )


def mul4(v, n):
    return pl.multiple_of(v * n, n)


def dot(a, b):
    return lax.dot_general(a, b, (((1,), (0,)), ((), ())), preferred_element_type=F32)


def call(kernel, idx, ins, outs, scratch=(), flops=0, limit_mib=16, name=None):
    specs = [pl.BlockSpec(memory_space=SMEM)] + [pl.BlockSpec(memory_space=VMEM) for _ in ins]
    single = not isinstance(outs, (list, tuple))
    shapes = [outs] if single else list(outs)
    got = pl.pallas_call(
        kernel,
        out_shape=shapes,
        in_specs=specs,
        out_specs=[pl.BlockSpec(memory_space=VMEM) for _ in shapes],
        scratch_shapes=list(scratch),
        compiler_params=pltpu.CompilerParams(vmem_limit_bytes=limit_mib << 20),
        cost_estimate=pl.CostEstimate(flops=flops, bytes_accessed=0, transcendentals=0),
        name=name,
    )(idx, *ins)
    return got[0] if single else got


def shaped(shape, dtype=BF16):
    return jax.ShapeDtypeStruct(shape, dtype)


def norm_kernel(idx, tokens, gain, w_rope, normed, rope_t):
    values = tokens[...].astype(F32)
    scale = lax.rsqrt(jnp.mean(values * values, axis=-1, keepdims=True) + EPS)
    out = (values * scale * gain[...]).astype(BF16)
    normed[...] = out
    rope_t[...] = dot(out, w_rope[...]).T.astype(BF16)


def dp_sum(idx, normed, mine, other):
    x, c = idx[2], idx[3]
    rows = mine[0].shape[0]
    total = None
    for i in range(RING):
        xi = lax.rem(x - i + RING, RING)
        for piece, core in ((mine[i][...], c), (other[i * rows : (i + 1) * rows, :], 1 - c)):
            left = normed[:, pl.ds(mul4(xi * CORES + core, rows), rows)]
            part = dot(left, piece)
            total = part if total is None else total + part
    return total


def latent_kernel(idx, normed, rope_t, gain, m0, m1, m2, m3, other, out_a, out_b):
    total = dp_sum(idx, normed, (m0, m1, m2, m3), other)
    scale = lax.rsqrt(jnp.mean(total * total, axis=-1, keepdims=True) + EPS)
    lat = (total * scale * gain[...]).T.astype(BF16)
    cut = out_a.shape[0]
    out_a[...] = lat[:cut]
    out_b[0 : lat.shape[0] - cut, :] = lat[cut:]
    out_b[lat.shape[0] - cut :, :] = rope_t[...]


def query_latent_kernel(idx, normed, gain, m0, m1, m2, m3, other, out):
    total = dp_sum(idx, normed, (m0, m1, m2, m3), other)
    scale = lax.rsqrt(jnp.mean(total * total, axis=-1, keepdims=True) + EPS)
    out[...] = (total * scale * gain[...]).T.astype(BF16)


def up_kernel(idx, mine, other, wq_t, wkv_t, wq, wkv):
    y, x, c = idx[1], idx[2], idx[3]
    for j in range(RING):
        hh = lax.rem(y - j + RING, RING)
        for i in range(RING):
            xi = lax.rem(x - i + RING, RING)
            at = (j * RING + i) * 96
            for ref, core in ((mine, c), (other, 1 - c)):
                d = xi * CORES + core
                wq[hh, pl.ds(mul4(d, 64), 64), :] = ref[at : at + 64, :]
                wkv[hh, pl.ds(mul4(d, 32), 32), :] = ref[at + 64 : at + 96, :]
    for h in range(RING):
        wq_t[h] = wq[h].astype(F32).T[:192].astype(BF16)
        wkv_t[h] = wkv[h].astype(F32).T.astype(BF16)


def order_kernel(idx, a0, a1, a2, a3, b0, b1, b2, b3, out):
    z, y = idx[0], idx[1]
    aa, bb = (a0, a1, a2, a3), (b0, b1, b2, b3)
    cut = a0.shape[0] // RING
    for k in range(RING):
        for j in range(RING):
            at = lax.rem(z - k + RING, RING) * RING + lax.rem(y - j + RING, RING)
            out[at, 0:cut, :] = aa[j][k * cut : (k + 1) * cut, :]
            out[at, cut : 2 * cut, :] = bb[k][j * cut : (j + 1) * cut, :]


def turned(rope, cosine, sine):
    first, second = rope[:HALF], rope[HALF:]
    return first * cosine - second * sine, second * cosine + first * sine


def head_kernel(hh, idx, kv, l0, l1, l2, l3, wq, wkv, cos, sin, qg, kg, o0, o1, o2, o3, ks, vs, ss):
    z, y = idx[0], idx[1]
    lats, outs = (l0, l1, l2, l3), (o0, o1, o2, o3)
    width = 192
    factor = (width**-0.5) * LOG2E
    wide = RING * BLOCK

    def build(b, _):
        up = dot(wkv[hh], kv[b, 0:256, :])
        key = up[:128]
        rope = kv[b, 256:320, :].astype(F32)
        square = jnp.sum(key * key, axis=0, keepdims=True) + jnp.sum(
            rope * rope, axis=0, keepdims=True
        )
        scale = lax.rsqrt(square / width + EPS)
        plain = key * scale * kg[0:128, :]
        r1, r2 = turned(rope * scale * kg[128:192, :], cos[b], sin[b])
        full = jnp.concatenate([plain, r1, r2, jnp.zeros((TAIL, BLOCK), F32)], axis=0)
        ks[pl.ds(mul4(b, BLOCK), BLOCK), :] = full.T.astype(BF16)
        vs[:, pl.ds(mul4(b, BLOCK), BLOCK)] = up[128:].astype(BF16)
        return 0

    lax.fori_loop(0, (RING - 1) * RING + y + 1, build, 0)
    key_at = lax.broadcasted_iota(jnp.int32, (BLOCK, BLOCK), 0)
    query_at = lax.broadcasted_iota(jnp.int32, (BLOCK, BLOCK), 1)

    for k in range(RING):
        zq = lax.rem(z + k, RING)
        block = zq * RING + y
        total = dot(wq[hh], lats[(RING - k) % RING][...])
        scale = lax.rsqrt(jnp.mean(total * total, axis=0, keepdims=True) + EPS)
        normal = total * scale * qg[...]
        r1, r2 = turned(normal[128:], cos[block], sin[block])
        query = jnp.concatenate(
            [normal[:128], r1, r2, jnp.zeros((TAIL, BLOCK), F32)], axis=0
        ).astype(BF16)

        def top(scores, best):
            return jnp.maximum(best, jnp.max(scores.reshape(-1, 8, BLOCK), axis=0))

        def first_wide(s, best):
            at = pl.ds(mul4(s, wide), wide)
            scores = dot(ks[at, :], query)
            ss[at, :] = scores
            return top(scores, best)

        def first_tail(j, best):
            at = pl.ds(mul4(zq * RING + j, BLOCK), BLOCK)
            scores = dot(ks[at, :], query)
            scores = jnp.where(key_at + (j - y) * BLOCK <= query_at, scores, NEG_BIG)
            ss[at, :] = scores
            return top(scores, best)

        best = jnp.full((8, BLOCK), NEG_BIG, F32)
        best = lax.fori_loop(0, zq, first_wide, best)
        best = lax.fori_loop(0, y + 1, first_tail, best)
        best = jnp.max(best, axis=0, keepdims=True)

        def second(at, carry):
            acc, mass = carry
            weight = jnp.exp2((ss[at, :] - best) * factor)
            mass = mass + jnp.sum(weight.reshape(-1, 8, BLOCK), axis=0)
            return acc + dot(vs[:, at], weight.astype(BF16)), mass

        carry = (jnp.zeros((128, BLOCK), F32), jnp.zeros((8, BLOCK), F32))
        carry = lax.fori_loop(0, zq, lambda s, v: second(pl.ds(mul4(s, wide), wide), v), carry)
        acc, mass = lax.fori_loop(
            0, y + 1, lambda j, v: second(pl.ds(mul4(zq * RING + j, BLOCK), BLOCK), v), carry
        )
        whole = jnp.sum(mass, axis=0, keepdims=True)
        outs[k][...] = (acc / whole).T.astype(BF16)


def out_rows_kernel(idx, m0, m1, m2, m3, s0, s1, s2, s3, out):
    z, y, x, c = idx[0], idx[1], idx[2], idx[3]
    mine, other = (m0, m1, m2, m3), (s0, s1, s2, s3)
    for i in range(RING):
        xi = lax.rem(x - i + RING, RING)
        for pieces, core in ((mine, c), (other, 1 - c)):
            for j in range(RING):
                for k in range(RING):
                    head = lax.rem(z - k + RING, RING) * RING + lax.rem(y - j + RING, RING)
                    to = mul4(head * RING * CORES + xi * CORES + core, 16)
                    at = (j * RING + k) * 16
                    out[pl.ds(to, 16), :] = pieces[i][at : at + 16, :]


def final_kernel(idx, *refs):
    parts, gain, w_out, out, mixed = refs[:16], refs[16], refs[17], refs[18], refs[19]
    z = idx[0]
    square = None
    for ref in parts:
        value = ref[...].astype(F32)
        one = jnp.sum(value * value, axis=-1, keepdims=True)
        square = one if square is None else square + one
    scale = lax.rsqrt(square / (HEADS * 128) + EPS)
    for n, ref in enumerate(parts):
        hh, k = n // RING, n % RING
        head = lax.rem(z - k + RING, RING) * RING + hh
        value = ref[...].astype(F32) * scale * gain[pl.ds(head, 1), :]
        mixed[:, pl.ds(mul4(head, 128), 128)] = value.astype(BF16)
    out[...] = dot(mixed[...], w_out[...]).astype(BF16)


def per_device(
    tokens,
    in_gain,
    w_query_down,
    w_latent_down,
    w_rope_key,
    query_latent_gain,
    latent_gain,
    w_query_up,
    w_key_up,
    w_value_up,
    query_gain,
    key_gain,
    out_gain,
    w_out,
):
    sp, dp = lax.axis_index("sp"), lax.axis_index("dp")
    idx = jnp.stack([sp // RING, sp % RING, dp // CORES, dp % CORES]).astype(jnp.int32)
    rows = tokens.reshape(tokens.shape[1], tokens.shape[2])
    count, model = rows.shape
    blocks = HEADS

    frequency = THETA ** (-jnp.arange(HALF, dtype=F32) / HALF)
    positions = jnp.arange(blocks * count, dtype=F32).reshape(blocks, 1, count)
    angles = positions * frequency[None, :, None]
    cosine, sine = jnp.cos(angles), jnp.sin(angles)

    lat_x = from_x(w_latent_down)
    lat_c = from_core(jnp.concatenate(lat_x, axis=0))

    pack = jnp.concatenate(
        [
            jnp.pad(w_query_up, ((0, 0), (0, 64))),
            jnp.concatenate([w_key_up, w_value_up], axis=1),
        ],
        axis=0,
    )
    up_x = jnp.concatenate(from_x(pack), axis=0)
    up_y = jnp.concatenate(from_y(up_x), axis=0)
    up_c = from_core(up_y)

    qd_x = from_x(w_query_down)
    qd_c = from_core(jnp.concatenate(qd_x, axis=0))

    out_z = jnp.concatenate(from_z(w_out), axis=0)
    out_y = jnp.concatenate(from_y(out_z), axis=0)
    out_y, _ = lax.optimization_barrier((out_y, qd_c))
    out_x = from_x(out_y)
    out_c = [from_core(piece) for piece in out_x]

    normed, rope_t = call(
        norm_kernel,
        idx,
        (rows, in_gain[None, :], w_rope_key),
        [shaped((count, model)), shaped((TAIL, count))],
        flops=10**9,
        name="norm",
    )
    lat_a, lat_b = call(
        latent_kernel,
        idx,
        (normed, rope_t, latent_gain[None, :], *lat_x, lat_c),
        [shaped((160, count)), shaped((160, count))],
        flops=10**9,
        name="latent",
    )
    a_z = jnp.concatenate(from_z(lat_a), axis=0)
    b_y = jnp.concatenate(from_y(lat_b), axis=0)
    a_all = from_y(a_z)
    b_all = from_z(b_y)

    lat_q = call(
        query_latent_kernel,
        idx,
        (normed, query_latent_gain[None, :], *qd_x, qd_c),
        shaped((512, count)),
        flops=10**9,
        name="query_latent",
    )
    q_all = from_z(lat_q)

    wq_t, wkv_t = call(
        up_kernel,
        idx,
        (up_y, up_c),
        [shaped((RING, 192, 512)), shaped((RING, 256, 256))],
        scratch=[pltpu.VMEM((RING, 512, 256), BF16), pltpu.VMEM((RING, 256, 256), BF16)],
        flops=10**9,
        name="up",
    )
    kv = call(
        order_kernel, idx, (*a_all, *b_all), shaped((blocks, 320, count)), flops=10**9, name="order"
    )

    parts = []
    for hh in range(RING):
        mine = call(
            lambda *refs, hh=hh: head_kernel(hh, *refs),
            idx,
            (kv, *q_all, wq_t, wkv_t, cosine, sine, query_gain[:, None], key_gain[:, None]),
            [shaped((count, 128))] * RING,
            scratch=[
                pltpu.VMEM((blocks * count, 256), BF16),
                pltpu.VMEM((128, blocks * count), BF16),
                pltpu.VMEM((blocks * count, count), F32),
            ],
            flops=4 * 10**9,
            limit_mib=24,
            name=f"head{hh}",
        )
        parts += [mine[0]] + [
            lax.ppermute(mine[k], "sp", sp_pairs(k, 0)) for k in range(1, RING)
        ]

    weights = call(
        out_rows_kernel,
        idx,
        (*out_x, *out_c),
        shaped((model, model)),
        flops=10**9,
        limit_mib=24,
        name="out_rows",
    )
    result = call(
        final_kernel,
        idx,
        (*parts, out_gain.reshape(HEADS, 128), weights),
        shaped((count, model)),
        scratch=[pltpu.VMEM((count, model), BF16)],
        flops=2 * 10**9,
        limit_mib=24,
        name="final",
    )
    return result.reshape(1, count, model)


def solution(mesh):
    in_specs = (
        P("dp", "sp", None),
        P(),
        P("dp", None),
        P("dp", None),
        P(),
        P(),
        P(),
        P("dp", "sp"),
        P("dp", "sp"),
        P("dp", "sp"),
        P(),
        P(),
        P(),
        P(("sp", "dp"), None),
    )
    out_specs = P("dp", "sp", None)
    return jax.shard_map(
        per_device, mesh=mesh, in_specs=in_specs, out_specs=out_specs, check_vma=False
    )
```

```python
import jax
import jax.numpy as jnp
from jax import lax
from jax.experimental import pallas as pl
from jax.experimental.pallas import tpu as pltpu
from jax.sharding import PartitionSpec as P


HEADS = 16
EPS = 1e-06
THETA = 10000.0
NEG_BIG = -1e30
LOG2E = 1.4426950408889634
F32 = jnp.float32
BF16 = jnp.bfloat16

RING = 4
CORES = 2
BLOCK = 256
TAIL = 64
HALF = TAIL // 2
WIDE = RING * BLOCK
STEPS = RING * (RING + 1) // 2
GROUPS = ((0, 1), (2, 3))
VMEM = pltpu.VMEM
SMEM = pltpu.SMEM


def sp_pairs(dz, dy):
    return [
        (z * RING + y, (z + dz) % RING * RING + (y + dy) % RING)
        for z in range(RING)
        for y in range(RING)
    ]


def dp_pairs(dx):
    return [
        (x * CORES + c, (x + dx) % RING * CORES + c) for x in range(RING) for c in range(CORES)
    ]


def from_z(value):
    return [value] + [lax.ppermute(value, "sp", sp_pairs(k, 0)) for k in range(1, RING)]


def from_y(value):
    return [value] + [lax.ppermute(value, "sp", sp_pairs(0, k)) for k in range(1, RING)]


def from_x(value):
    return [value] + [lax.ppermute(value, "dp", dp_pairs(k)) for k in range(1, RING)]


def from_core(value):
    return lax.ppermute(
        value, "dp", [(x * CORES + c, x * CORES + 1 - c) for x in range(RING) for c in range(CORES)]
    )


def mul4(v, n):
    return pl.multiple_of(v * n, n)


def dot(a, b):
    return lax.dot_general(a, b, (((1,), (0,)), ((), ())), preferred_element_type=F32)


def call(kernel, idx, ins, outs, scratch=(), flops=0, limit_mib=16, name=None):
    specs = [pl.BlockSpec(memory_space=SMEM)] + [pl.BlockSpec(memory_space=VMEM) for _ in ins]
    single = not isinstance(outs, (list, tuple))
    shapes = [outs] if single else list(outs)
    got = pl.pallas_call(
        kernel,
        out_shape=shapes,
        in_specs=specs,
        out_specs=[pl.BlockSpec(memory_space=VMEM) for _ in shapes],
        scratch_shapes=list(scratch),
        compiler_params=pltpu.CompilerParams(vmem_limit_bytes=limit_mib << 20),
        cost_estimate=pl.CostEstimate(flops=flops, bytes_accessed=0, transcendentals=0),
        name=name,
    )(idx, *ins)
    return got[0] if single else got


def shaped(shape, dtype=BF16):
    return jax.ShapeDtypeStruct(shape, dtype)


def norm_kernel(idx, tokens, gain, w_rope, normed, rope_t):
    values = tokens[...].astype(F32)
    scale = lax.rsqrt(jnp.mean(values * values, axis=-1, keepdims=True) + EPS)
    out = (values * scale * gain[...]).astype(BF16)
    normed[...] = out
    rope_t[...] = dot(out, w_rope[...]).T.astype(BF16)


def dp_sum(idx, normed, mine, other):
    x, c = idx[2], idx[3]
    rows = mine[0].shape[0]
    total = None
    for i in range(RING):
        xi = lax.rem(x - i + RING, RING)
        for piece, core in ((mine[i][...], c), (other[i][...], 1 - c)):
            left = normed[:, pl.ds(mul4(xi * CORES + core, rows), rows)]
            part = dot(left, piece)
            total = part if total is None else total + part
    return total


def latent_kernel(idx, normed, rope_t, gain, m0, m1, m2, m3, s0, s1, s2, s3, out_a, out_b):
    total = dp_sum(idx, normed, (m0, m1, m2, m3), (s0, s1, s2, s3))
    scale = lax.rsqrt(jnp.mean(total * total, axis=-1, keepdims=True) + EPS)
    lat = (total * scale * gain[...]).T.astype(BF16)
    cut = out_a.shape[0]
    out_a[...] = lat[:cut]
    out_b[0 : lat.shape[0] - cut, :] = lat[cut:]
    out_b[lat.shape[0] - cut :, :] = rope_t[...]


def query_latent_kernel(idx, normed, gain, m0, m1, m2, m3, s0, s1, s2, s3, out):
    total = dp_sum(idx, normed, (m0, m1, m2, m3), (s0, s1, s2, s3))
    scale = lax.rsqrt(jnp.mean(total * total, axis=-1, keepdims=True) + EPS)
    out[...] = (total * scale * gain[...]).T.astype(BF16)


def join_kernel(idx, *refs):
    rows = refs[0].shape[0]
    for n, ref in enumerate(refs[:-1]):
        refs[-1][n * rows : (n + 1) * rows, :] = ref[...]


def up_kernel(idx, m0, m1, m2, m3, s0, s1, s2, s3, wq_t, wkv_t, wq, wkv):
    y, x, c = idx[1], idx[2], idx[3]
    for i in range(RING):
        xi = lax.rem(x - i + RING, RING)
        for ref, core in (((m0, m1, m2, m3)[i], c), ((s0, s1, s2, s3)[i], 1 - c)):
            d = xi * CORES + core
            for j in range(RING):
                hh = lax.rem(y - j + RING, RING)
                at = j * 96
                wq[hh, pl.ds(mul4(d, 64), 64), :] = ref[at : at + 64, :]
                wkv[hh, pl.ds(mul4(d, 32), 32), :] = ref[at + 64 : at + 96, :]
    for h in range(RING):
        wq_t[h] = wq[h].astype(F32).T[:192].astype(BF16)
        wkv_t[h] = wkv[h].astype(F32).T.astype(BF16)


def order_kernel(idx, a0, a1, a2, a3, b0, b1, b2, b3, out):
    z, y = idx[0], idx[1]
    aa, bb = (a0, a1, a2, a3), (b0, b1, b2, b3)
    cut = a0.shape[0] // RING
    for k in range(RING):
        for j in range(RING):
            at = lax.rem(z - k + RING, RING) * RING + lax.rem(y - j + RING, RING)
            to = pl.ds(mul4(at, BLOCK), BLOCK)
            out[0:cut, to] = aa[j][k * cut : (k + 1) * cut, :]
            out[cut : 2 * cut, to] = bb[k][j * cut : (j + 1) * cut, :]


def turned(rope, cosine, sine):
    first, second = rope[:HALF], rope[HALF:]
    return first * cosine - second * sine, second * cosine + first * sine


def query_kernel(idx, l0, l1, l2, l3, wq, cos, sin, qg, out):
    z, y = idx[0], idx[1]
    lats = (l0, l1, l2, l3)
    for k in range(RING):
        block = lax.rem(z + k, RING) * RING + y
        at = pl.ds(mul4(block, BLOCK), BLOCK)
        for h in range(RING):
            total = dot(wq[h], lats[(RING - k) % RING][...])
            scale = lax.rsqrt(jnp.mean(total * total, axis=0, keepdims=True) + EPS)
            normal = total * scale * qg[...]
            r1, r2 = turned(normal[128:], cos[:, at], sin[:, at])
            out[h * RING + k] = jnp.concatenate(
                [normal[:128], r1, r2, jnp.zeros((TAIL, BLOCK), F32)], axis=0
            ).astype(BF16)


def head_kernel(heads, idx, kv, qs, wkv, cos, sin, kg, *rest):
    outs = rest[:RING]
    ks, vs, ss, bias, acc, mx, ms, done = rest[RING:]
    y = idx[1]
    width = 192
    factor = (width**-0.5) * LOG2E
    length = kv.shape[1]
    key_at = lax.broadcasted_iota(jnp.int32, (WIDE, BLOCK), 0)
    query_at = lax.broadcasted_iota(jnp.int32, (WIDE, BLOCK), 1)
    bias[0:WIDE, :] = jnp.zeros((WIDE, BLOCK), F32)
    bias[WIDE : 2 * WIDE, :] = jnp.where(key_at <= query_at + y * BLOCK, 0.0, NEG_BIG)
    acc[...] = jnp.zeros((128, BLOCK), F32)
    ms[...] = jnp.zeros((8, BLOCK), F32)

    for n, hh in enumerate(heads):

        def build(b, _, n=n, hh=hh):
            at = pl.ds(mul4(b, WIDE), WIDE)
            up = dot(wkv[hh], kv[0:256, at])
            key = up[:128]
            rope = kv[256:320, at].astype(F32)
            square = jnp.sum(key * key, axis=0, keepdims=True) + jnp.sum(
                rope * rope, axis=0, keepdims=True
            )
            scale = lax.rsqrt(square / width + EPS)
            plain = key * scale * kg[0:128, :]
            r1, r2 = turned(rope * scale * kg[128:192, :], cos[:, at], sin[:, at])
            full = jnp.concatenate([plain, r1, r2, jnp.zeros((TAIL, WIDE), F32)], axis=0)
            ks[pl.ds(mul4(b + n * (length // WIDE), WIDE), WIDE), :] = full.astype(BF16).T
            vs[n, :, at] = up[128:].astype(BF16)
            return 0

        lax.fori_loop(0, length // WIDE, build, 0)

    steps = STEPS * len(heads)

    def where_is(t):
        u = lax.rem(t, STEPS)
        return t // STEPS, idx[4 + u], idx[4 + STEPS + u], idx[4 + 2 * STEPS + u]

    def score(n, k, s, last, r):
        row = pl.ds(mul4(n * (length // WIDE) + s, WIDE) + r * BLOCK, BLOCK)
        scores = dot(ks[row, :], qs[(n + heads[0]) * RING + k])
        scores = scores + bias[pl.ds(mul4(last, WIDE) + r * BLOCK, BLOCK), :]
        ss[r * BLOCK : (r + 1) * BLOCK, :] = scores
        return jnp.max(scores.reshape(-1, 8, BLOCK), axis=0)

    def step(t, best):
        ahead = where_is(lax.rem(t, steps))
        n, k, s, last = where_is(t - 1)
        old = jnp.where(s == 0, NEG_BIG, mx[0:1, :])
        new = jnp.maximum(old, jnp.max(best, axis=0, keepdims=True))
        mx[0:1, :] = new
        shrink = jnp.exp2((old - new) * factor)
        total, mass, fresh = None, None, None
        for r in range(RING):
            weight = jnp.exp2((ss[r * BLOCK : (r + 1) * BLOCK, :] - new) * factor)
            one = jnp.sum(weight.reshape(-1, 8, BLOCK), axis=0)
            part = dot(vs[n, :, pl.ds(mul4(s, WIDE) + r * BLOCK, BLOCK)], weight.astype(BF16))
            top = score(*ahead, r)
            mass = one if mass is None else mass + one
            total = part if total is None else total + part
            fresh = top if fresh is None else jnp.maximum(fresh, top)
        acc[...] = acc[...] * shrink + total
        ms[...] = ms[...] * shrink + mass

        @pl.when(last == 1)
        def _():
            whole = jnp.sum(ms[...], axis=0, keepdims=True)
            done[n * RING + k] = (acc[...] / whole).T.astype(BF16)

        return fresh

    first = None
    for r in range(RING):
        top = score(*where_is(0), r)
        first = top if first is None else jnp.maximum(first, top)
    lax.fori_loop(1, steps + 1, step, first)
    for n in range(len(heads)):
        for k in range(RING):
            outs[k][n * BLOCK : (n + 1) * BLOCK, :] = done[n * RING + k]


def out_rows_kernel(idx, m0, m1, m2, m3, s0, s1, s2, s3, out):
    z, y, x, c = idx[0], idx[1], idx[2], idx[3]
    mine, other = (m0, m1, m2, m3), (s0, s1, s2, s3)
    for i in range(RING):
        xi = lax.rem(x - i + RING, RING)
        for pieces, core in ((mine, c), (other, 1 - c)):
            for j in range(RING):
                for k in range(RING):
                    head = lax.rem(z - k + RING, RING) * RING + lax.rem(y - j + RING, RING)
                    to = mul4(head * RING * CORES + xi * CORES + core, 16)
                    at = (j * RING + k) * 16
                    out[pl.ds(to, 16), :] = pieces[i][at : at + 16, :]


def final_kernel(groups, idx, *refs):
    count = RING * len(groups)
    parts, gain, w_out, out, mixed = refs[:count], *refs[count:]
    z = idx[0]
    pieces = []
    for g, heads in enumerate(groups):
        for k in range(RING):
            for n, hh in enumerate(heads):
                head = lax.rem(z - k + RING, RING) * RING + hh
                pieces.append((parts[g * RING + k], slice(n * BLOCK, (n + 1) * BLOCK), head))
    square = None
    for ref, rows, _ in pieces:
        value = ref[rows, :].astype(F32)
        one = jnp.sum(value * value, axis=-1, keepdims=True)
        square = one if square is None else square + one
    scale = lax.rsqrt(square / (HEADS * 128) + EPS)
    for ref, rows, head in pieces:
        value = ref[rows, :].astype(F32) * scale * gain[pl.ds(head, 1), :]
        mixed[:, pl.ds(mul4(head, 128), 128)] = value.astype(BF16)
    out[...] = dot(mixed[...], w_out[...]).astype(BF16)


def per_device(
    tokens,
    in_gain,
    w_query_down,
    w_latent_down,
    w_rope_key,
    query_latent_gain,
    latent_gain,
    w_query_up,
    w_key_up,
    w_value_up,
    query_gain,
    key_gain,
    out_gain,
    w_out,
):
    sp, dp = lax.axis_index("sp"), lax.axis_index("dp")
    idx = jnp.stack([sp // RING, sp % RING, dp // CORES, dp % CORES]).astype(jnp.int32)
    rows = tokens.reshape(tokens.shape[1], tokens.shape[2])
    count, model = rows.shape

    table = []
    for z in range(RING):
        steps = [(k, n, int(n == (z + k) % RING)) for k in range(RING) for n in range((z + k) % RING + 1)]
        table.append([one[i] for i in range(3) for one in steps])
    idx = jnp.concatenate([idx, jnp.array(table, jnp.int32)[sp // RING]])

    frequency = THETA ** (-jnp.arange(HALF, dtype=F32) / HALF)
    positions = jnp.arange(HEADS * count, dtype=F32)
    angles = positions[None, :] * frequency[:, None]
    cosine, sine = jnp.cos(angles), jnp.sin(angles)

    def join(pieces, name):
        rows_of, width = pieces[0].shape
        return call(
            join_kernel, idx, pieces, shaped((rows_of * len(pieces), width)), flops=10**8, name=name
        )

    lat_x = from_x(w_latent_down)
    lat_c = [from_core(piece) for piece in lat_x]
    qd_x = from_x(w_query_down)
    qd_c = [from_core(piece) for piece in qd_x]

    pack = jnp.concatenate(
        [
            jnp.pad(w_query_up, ((0, 0), (0, 64))),
            jnp.concatenate([w_key_up, w_value_up], axis=1),
        ],
        axis=0,
    )
    up_y = join(from_y(pack), "up_join")
    up_x = from_x(up_y)
    up_c = [from_core(piece) for piece in up_x]

    out_z = join(from_z(w_out), "out_join_z")
    out_y = join(from_y(out_z), "out_join_y")
    out_y, _ = lax.optimization_barrier((out_y, (qd_x, up_x)))
    out_x = from_x(out_y)
    out_c = [from_core(piece) for piece in out_x]

    normed, rope_t = call(
        norm_kernel,
        idx,
        (rows, in_gain[None, :], w_rope_key),
        [shaped((count, model)), shaped((TAIL, count))],
        flops=10**9,
        name="norm",
    )
    lat_a, lat_b = call(
        latent_kernel,
        idx,
        (normed, rope_t, latent_gain[None, :], *lat_x, *lat_c),
        [shaped((160, count)), shaped((160, count))],
        flops=10**9,
        name="latent",
    )
    a_z = join(from_z(lat_a), "a_join")
    b_y = join(from_y(lat_b), "b_join")
    a_all = from_y(a_z)
    b_all = from_z(b_y)

    lat_q = call(
        query_latent_kernel,
        idx,
        (normed, query_latent_gain[None, :], *qd_x, *qd_c),
        shaped((512, count)),
        flops=10**9,
        name="query_latent",
    )
    q_all = from_z(lat_q)

    wq_t, wkv_t = call(
        up_kernel,
        idx,
        (*up_x, *up_c),
        [shaped((RING, 192, 512)), shaped((RING, 256, 256))],
        scratch=[pltpu.VMEM((RING, 512, 256), BF16), pltpu.VMEM((RING, 256, 256), BF16)],
        flops=10**9,
        name="up",
    )
    queries = call(
        query_kernel,
        idx,
        (*q_all, wq_t, cosine, sine, query_gain[:, None]),
        shaped((HEADS, 256, count)),
        flops=10**9,
        name="queries",
    )
    kv = call(
        order_kernel, idx, (*a_all, *b_all), shaped((320, HEADS * count)), flops=10**9, name="order"
    )

    parts = []
    for heads in GROUPS:
        many = len(heads)
        mine = call(
            lambda *refs, heads=heads: head_kernel(heads, *refs),
            idx,
            (kv, queries, wkv_t, cosine, sine, key_gain[:, None]),
            [shaped((many * count, 128))] * RING,
            scratch=[
                pltpu.VMEM((many * HEADS * count, 256), BF16),
                pltpu.VMEM((many, 128, HEADS * count), BF16),
                pltpu.VMEM((WIDE, BLOCK), F32),
                pltpu.VMEM((2 * WIDE, BLOCK), F32),
                pltpu.VMEM((128, BLOCK), F32),
                pltpu.VMEM((8, BLOCK), F32),
                pltpu.VMEM((8, BLOCK), F32),
                pltpu.VMEM((many * RING, BLOCK, 128), BF16),
            ],
            flops=many * 4 * 10**9,
            limit_mib=30,
            name=f"heads{heads[0]}",
        )
        parts += [mine[0]] + [
            lax.ppermute(mine[k], "sp", sp_pairs(k, 0)) for k in range(1, RING)
        ]

    weights = call(
        out_rows_kernel,
        idx,
        (*out_x, *out_c),
        shaped((model, model)),
        flops=10**9,
        limit_mib=24,
        name="out_rows",
    )
    result = call(
        lambda *refs: final_kernel(GROUPS, *refs),
        idx,
        (*parts, out_gain.reshape(HEADS, 128), weights),
        shaped((count, model)),
        scratch=[pltpu.VMEM((count, model), BF16)],
        flops=2 * 10**9,
        limit_mib=24,
        name="final",
    )
    return result.reshape(1, count, model)


def solution(mesh):
    in_specs = (
        P("dp", "sp", None),
        P(),
        P("dp", None),
        P("dp", None),
        P(),
        P(),
        P(),
        P("dp", "sp"),
        P("dp", "sp"),
        P("dp", "sp"),
        P(),
        P(),
        P(),
        P(("sp", "dp"), None),
    )
    out_specs = P("dp", "sp", None)
    return jax.shard_map(
        per_device, mesh=mesh, in_specs=in_specs, out_specs=out_specs, check_vma=False
    )
```
